32 devices in a mesh: st: 16 (over z, y, x), tp: 2 (over core).
Axes of the slice: x: 2, y: 2, z: 4, core: 2. Of those that a mesh axis runs over, the one named last changes fastest.
Arguments:
- hidden: bfloat16 [8192, 2048], P('st'), may hold values from -24 to 24
- passage_store: bfloat16 [512, 64, 2048], P('st'), may hold values from -6 to 6
- passage_ids: int32 [128, 4], P('st'), may hold values from 0 to 511, as said below
- query_weight: bfloat16 [2048, 512], P(None, 'tp'), may hold values from -0.125 to 0.125
- gate_weight: bfloat16 [2048, 512], P(None, 'tp'), may hold values from -0.125 to 0.125
- key_weight: bfloat16 [2048, 512], P(None, 'tp'), may hold values from -0.125 to 0.125
- value_weight: bfloat16 [2048, 512], P(None, 'tp'), may hold values from -0.125 to 0.125
- output_grad: bfloat16 [8192, 512], P('st', 'tp'), may hold values from -6 to 6
Outputs:
- grad_hidden: bfloat16 [8192, 2048], P(('st', 'tp'))
- grad_store: bfloat16 [512, 64, 2048], P(('st', 'tp'))
- grad_value_weight: float32 [2048, 512], P(None, 'tp')
The draws below stay inside these ranges and needn't reach their ends.
Inputs may be any that keep to these rules, and one draw needn't show every extreme that they name: `passage_ids`: passage p is held at st index p // 32. The 32 ids of one index of st (its 8 blocks) are distinct; at most 4 of them name passages of one owner, and on every index some owner is named exactly 4 times. Every index reads at least one passage of the owner before it, of the owner after it and of the owner half the axis away.
All inputs are finite; a program needn't handle non-finite values.
Results may differ from the reference program's by a relative error of at most 0.012.
The reference program's roundings to bfloat16 on the way count: a program that leaves them out, or rounds other values in their place, can miss the bound.
Values may be sent and summed in bfloat16 or wider, within the bound.
A program may use at most 128 MiB of HBM per device.

```python
import jax
import jax.numpy as jnp
from jax import lax

D = 2048
HEADS = 2
HEAD_DIM = 256
MW = 512
BLK = 64
NP = 4
PLEN = 64
P_DEV = 32
TOKENS = 8192
PASSAGES = 512
NB_DEV = 8
NBLK = 128
REQ_DEV = 32
CAP = 4


def draw_hidden(key, part):
    keys_three = jax.random.split(key, 3)
    drawn = jnp.clip(jax.random.normal(keys_three[0], (TOKENS, D), jnp.float32), -6.0, 6.0)
    return drawn.astype(jnp.bfloat16)


def draw_passage_ids(key, part):
    owner_total = PASSAGES // P_DEV
    slot_total = owner_total * CAP

    def one_source(source_key, source):
        split_keys = jax.random.split(source_key, 4)
        slot_iota = jnp.arange(slot_total, dtype=jnp.int32)
        slot_owner = slot_iota // CAP
        slot_rank = slot_iota % CAP
        shuffled = jax.random.permutation(split_keys[0], slot_total).astype(jnp.int32)
        before = (source + owner_total - 1) % owner_total
        after = (source + 1) % owner_total
        across = (source + owner_total // 2) % owner_total
        score = jnp.where(slot_owner == before, slot_rank, shuffled + 2 * slot_total)
        score = jnp.where((slot_owner == across) & (slot_rank == 0), CAP, score)
        score = jnp.where((slot_owner == after) & (slot_rank == 0), CAP + 1, score)
        chosen = jnp.argsort(score, stable=True)[:REQ_DEV].astype(jnp.int32)
        chosen_owner = chosen // CAP
        chosen_rank = chosen % CAP
        first_pick = jax.random.randint(split_keys[1], (owner_total,), 0, P_DEV)
        second_pick = jax.random.randint(split_keys[2], (owner_total,), 0, P_DEV)
        popular = jnp.minimum(first_pick, second_pick)
        local_index = (popular[chosen_owner] + chosen_rank) % P_DEV
        ids_flat = jax.random.permutation(split_keys[3], chosen_owner * P_DEV + local_index)
        return ids_flat.reshape(NB_DEV, NP).astype(jnp.int32)
    source_keys = jax.random.split(key, owner_total)
    return jax.vmap(one_source)(source_keys, jnp.arange(owner_total, dtype=jnp.int32)).reshape(NBLK, NP)


def level_of(stream_key, extent, cuts, smallest, largest):
    def one(axis_at, parts):
        heights = jax.random.uniform(jax.random.fold_in(jax.random.fold_in(stream_key, 6), axis_at), (parts,), jnp.float32, smallest / len(cuts), largest / len(cuts))
        return jnp.repeat(jnp.exp(heights), extent[axis_at] // parts).reshape((-1,) + (1,) * (len(extent) - axis_at - 1))

    factor_of = one(*cuts[0])
    for cut in cuts[1:]:
        factor_of = factor_of * one(*cut)
    return factor_of


def noise(rng, extent, width, reach, cuts=(), kind=jnp.bfloat16):
    array = width * jax.random.normal(rng, extent, jnp.float32)
    if cuts:
        array = array * level_of(rng, extent, cuts, -0.22, 0.18)
    return jnp.clip(array, -reach, reach).astype(kind)


def setup_inputs(seed: int = 0) -> dict:
    key_list = jax.random.split(jax.random.key(seed), 9)
    return {
        "hidden": draw_hidden(jax.random.fold_in(key_list[8], 71), 0),
        "passage_store": noise(key_list[1], (PASSAGES, PLEN, D), 1.0, 6.0, ((0, 16),)),
        "passage_ids": draw_passage_ids(jax.random.fold_in(key_list[8], 71), 0),
        "query_weight": noise(key_list[3], (D, MW), D ** -0.5, 0.125, ((1, 2),)),
        "gate_weight": noise(key_list[4], (D, MW), D ** -0.5, 0.125, ((1, 2),)),
        "key_weight": noise(key_list[5], (D, MW), D ** -0.5, 0.125, ((1, 2),)),
        "value_weight": noise(key_list[6], (D, MW), D ** -0.5, 0.125, ((1, 2),)),
        "output_grad": noise(key_list[7], (TOKENS, MW), 1.0, 6.0, ((0, 16), (1, 2))),
    }


def block_grads(operands):
    query_block, gate_block, upstream_block, key_block, value_block = operands
    score_scale = HEAD_DIM ** -0.5
    query_heads = query_block.astype(jnp.float32).reshape(BLK, HEADS, HEAD_DIM)
    key_heads = key_block.astype(jnp.float32).reshape(NP * PLEN, HEADS, HEAD_DIM)
    value_heads = value_block.astype(jnp.float32).reshape(NP * PLEN, HEADS, HEAD_DIM)
    scores = jnp.einsum('qhd,khd->hqk', query_heads, key_heads) * score_scale
    probs = jax.nn.softmax(scores, axis=-1)
    probs_low = probs.astype(jnp.bfloat16)
    attended = jnp.einsum('hqk,khd->qhd', probs_low.astype(jnp.float32), value_heads).reshape(BLK, MW)
    gate_sigmoid = jax.nn.sigmoid(gate_block)
    upstream = upstream_block.astype(jnp.float32)
    d_attended = (upstream * gate_block * gate_sigmoid).astype(jnp.bfloat16)
    d_gates = (upstream * attended * gate_sigmoid * (1.0 + gate_block * (1.0 - gate_sigmoid))).astype(jnp.bfloat16)
    d_heads = d_attended.astype(jnp.float32).reshape(BLK, HEADS, HEAD_DIM)
    d_probs = jnp.einsum('qhd,khd->hqk', d_heads, value_heads)
    centre = jnp.sum(probs * d_probs, axis=-1, keepdims=True)
    d_scores = (probs * (d_probs - centre) * score_scale).astype(jnp.bfloat16).astype(jnp.float32)
    d_queries = jnp.einsum('hqk,khd->qhd', d_scores, key_heads).reshape(BLK, MW).astype(jnp.bfloat16)
    d_block_keys = jnp.einsum('hqk,qhd->khd', d_scores, query_heads).reshape(NP, PLEN, MW)
    d_block_values = jnp.einsum('hqk,qhd->khd', probs_low.astype(jnp.float32), d_heads).reshape(NP, PLEN, MW)
    return d_queries, d_gates, d_block_keys, d_block_values


def reference(hidden, passage_store, passage_ids, query_weight, gate_weight, key_weight, value_weight, output_grad):
    store_rows = passage_store.reshape(PASSAGES * PLEN, D)
    keys = jnp.dot(store_rows, key_weight, preferred_element_type=jnp.float32).astype(jnp.bfloat16).reshape(PASSAGES, PLEN, MW)
    values = jnp.dot(store_rows, value_weight, preferred_element_type=jnp.float32).astype(jnp.bfloat16).reshape(PASSAGES, PLEN, MW)
    queries = jnp.dot(hidden, query_weight, preferred_element_type=jnp.float32).astype(jnp.bfloat16).reshape(NBLK, BLK, MW)
    gates = jnp.dot(hidden, gate_weight, preferred_element_type=jnp.float32).reshape(NBLK, BLK, MW)
    flat_ids = passage_ids.reshape(NBLK * NP).astype(jnp.int32)
    key_blocks = keys[flat_ids].reshape(NBLK, NP * PLEN, MW)
    value_blocks = values[flat_ids].reshape(NBLK, NP * PLEN, MW)
    d_queries, d_gates, d_block_keys, d_block_values = lax.map(
        block_grads, (queries, gates, output_grad.reshape(NBLK, BLK, MW), key_blocks, value_blocks))
    d_queries = d_queries.reshape(TOKENS, MW)
    d_gates = d_gates.reshape(TOKENS, MW)
    grad_hidden = (jnp.dot(d_queries, query_weight.T, preferred_element_type=jnp.float32)
                   + jnp.dot(d_gates, gate_weight.T, preferred_element_type=jnp.float32)).astype(jnp.bfloat16)
    key_totals = jnp.zeros((PASSAGES, PLEN, MW), jnp.float32).at[flat_ids].add(d_block_keys.reshape(NBLK * NP, PLEN, MW))
    value_totals = jnp.zeros((PASSAGES, PLEN, MW), jnp.float32).at[flat_ids].add(d_block_values.reshape(NBLK * NP, PLEN, MW))
    key_low = key_totals.astype(jnp.bfloat16).reshape(PASSAGES * PLEN, MW)
    value_low = value_totals.astype(jnp.bfloat16).reshape(PASSAGES * PLEN, MW)
    grad_store = (jnp.dot(key_low, key_weight.T, preferred_element_type=jnp.float32)
                  + jnp.dot(value_low, value_weight.T, preferred_element_type=jnp.float32)).astype(jnp.bfloat16).reshape(PASSAGES, PLEN, D)
    grad_value_weight = jnp.dot(store_rows.T, value_low, preferred_element_type=jnp.float32)
    return grad_hidden, grad_store, grad_value_weight
```

```python
import functools

import jax
import jax.numpy as jnp
from jax import lax
from jax.experimental import pallas as pl
from jax.experimental.pallas import tpu as pltpu
from jax.sharding import PartitionSpec as P

HEAD_DIM = 256
NT = (((1,), (1,)), ((), ()))
TN = (((0,), (0,)), ((), ()))


def attend_kernel(per_block, span, heads, flat_ref, q_ref, gate_ref, up_ref, da_ref, k_ref, v_ref, dq_ref, dg_ref, out_ref):
    b = pl.program_id(0)

    @pl.when(b == 0)
    def _():
        out_ref[...] = jnp.zeros_like(out_ref)

    score_scale = HEAD_DIM ** (-0.5)
    slots = [flat_ref[b * per_block + j] for j in range(per_block)]
    keys = jnp.concatenate([k_ref[s] for s in slots], axis=0)
    values = jnp.concatenate([v_ref[s] for s in slots], axis=0)
    for h in range(heads):
        cols = slice(h * HEAD_DIM, (h + 1) * HEAD_DIM)
        k, v = keys[:, cols], values[:, cols]
        q, da = q_ref[:, cols], da_ref[:, cols]
        scores = lax.dot_general(q, k, NT, preferred_element_type=jnp.float32) * score_scale
        top = jnp.max(scores, axis=-1, keepdims=True)
        e = jnp.exp(scores - top)
        probs = e / jnp.sum(e, axis=-1, keepdims=True)
        attended = jnp.dot(probs.astype(jnp.bfloat16), v, preferred_element_type=jnp.float32)
        gates = gate_ref[:, cols]
        s = jax.nn.sigmoid(gates)
        up = up_ref[:, cols].astype(jnp.float32)
        dg_ref[:, cols] = (up * attended * s * (1.0 + gates * (1.0 - s))).astype(jnp.bfloat16)
        d_probs = lax.dot_general(da, v, NT, preferred_element_type=jnp.float32)
        centre = jnp.sum(probs * d_probs, axis=-1, keepdims=True)
        d_scores = probs * (d_probs - centre) * score_scale
        dq_ref[:, cols] = jnp.dot(
            d_scores.astype(jnp.bfloat16), k, preferred_element_type=jnp.float32
        ).astype(jnp.bfloat16)
        for j, slot in enumerate(slots):
            rows = slice(j * span, (j + 1) * span)
            out_ref[slot, :, h * 2 * span : (h + 1) * 2 * span] = jnp.concatenate(
                [probs[:, rows], d_scores[:, rows]], axis=1
            ).astype(jnp.bfloat16)


def totals_kernel(unroll, heads, held, span, passage_ref, row_ref, pd_ref, *rest):
    del row_ref
    g_refs = rest[:unroll]
    kt_ref, vt_ref, acc_k, acc_v = rest[unroll:]
    step = pl.program_id(0)
    width = heads * HEAD_DIM

    @pl.when(step == 0)
    def _():
        acc_k[...] = jnp.zeros_like(acc_k)
        acc_v[...] = jnp.zeros_like(acc_v)

    for u in range(unroll):
        p = passage_ref[step * unroll + u]
        for h in range(heads):
            cols = slice(h * HEAD_DIM, (h + 1) * HEAD_DIM)
            a = pd_ref[u, :, h * 2 * span : (h + 1) * 2 * span]
            both = jnp.concatenate(
                [g_refs[u][0, :, cols], g_refs[u][0, :, width + h * HEAD_DIM : width + (h + 1) * HEAD_DIM]],
                axis=1,
            )
            r = lax.dot_general(a, both, TN, preferred_element_type=jnp.float32)
            acc_v[p, :, cols] += r[:span, HEAD_DIM:]
            acc_k[p, :, cols] += r[span:, :HEAD_DIM]

    @pl.when(step == pl.num_programs(0) - 1)
    def _():
        kt_ref[...] = acc_k[:held].astype(jnp.bfloat16)
        vt_ref[...] = acc_v[:held].astype(jnp.bfloat16)


def body(
    hidden,
    passage_store,
    passage_ids,
    query_weight,
    gate_weight,
    key_weight,
    value_weight,
    output_grad,
):
    owner_count = lax.axis_size("st")
    tp_count = lax.axis_size("tp")
    tp_index = lax.axis_index("tp")
    held, span, model_width = passage_store.shape
    block_count, per_block = passage_ids.shape
    requests = block_count * per_block
    capacity = max(1, 2 * requests // owner_count)
    slot_total = owner_count * capacity
    width = query_weight.shape[1]
    heads = width // HEAD_DIM
    tokens = hidden.shape[0]
    block_rows = tokens // block_count
    bf16, f32 = jnp.bfloat16, jnp.float32
    exchange = [(i, tp_count - 1 - i) for i in range(tp_count)]

    ids = passage_ids.reshape(requests)
    owner_of = ids // held
    local_index = ids % held
    positions = jnp.arange(requests, dtype=jnp.int32)
    earlier = positions[None, :] < positions[:, None]
    rank = jnp.sum((owner_of[:, None] == owner_of[None, :]) & earlier, axis=1, dtype=jnp.int32)
    slot_flat = owner_of * capacity + rank
    code = local_index * block_count + positions // per_block + 1
    hit = slot_flat[:, None] == jnp.arange(slot_total, dtype=jnp.int32)[None, :]
    table = jnp.sum(jnp.where(hit, code[:, None], 0), axis=0, dtype=jnp.int32)
    came = lax.all_to_all(
        table.reshape(owner_count, capacity), "st", split_axis=0, concat_axis=0, tiled=True
    ).reshape(slot_total)
    filled = came > 0
    came0 = jnp.maximum(came - 1, 0)
    slot_passage = came0 // block_count
    slot_target = jnp.where(filled, slot_passage, held).astype(jnp.int32)
    reader = jnp.arange(slot_total, dtype=jnp.int32) // capacity
    slot_row = (reader * block_count + came0 % block_count).astype(jnp.int32)

    store_rows = passage_store.reshape(held * span, model_width)

    def project(rows, weight):
        return jnp.dot(rows, weight, preferred_element_type=f32)

    keys_here = project(store_rows, key_weight).astype(bf16).reshape(held, span, width)
    values_here = project(store_rows, value_weight).astype(bf16).reshape(held, span, width)
    came_keys = lax.all_to_all(
        keys_here[slot_passage].reshape(owner_count, capacity, span, width),
        "st", split_axis=0, concat_axis=0, tiled=True,
    ).reshape(slot_total, span, width)
    came_values = lax.all_to_all(
        values_here[slot_passage].reshape(owner_count, capacity, span, width),
        "st", split_axis=0, concat_axis=0, tiled=True,
    ).reshape(slot_total, span, width)

    queries = project(hidden, query_weight).astype(bf16)
    gates = project(hidden, gate_weight)
    d_attended = (output_grad.astype(f32) * gates * jax.nn.sigmoid(gates)).astype(bf16)
    shared = lax.all_gather(
        jnp.concatenate([queries, d_attended], axis=1), "st", axis=0, tiled=True
    ).reshape(owner_count * block_count, block_rows, 2 * width)

    token_weight = jnp.concatenate([query_weight, gate_weight], axis=1)
    token_weight = jnp.concatenate(
        [token_weight, lax.ppermute(token_weight, "tp", exchange)], axis=1
    )
    row_weight = jnp.concatenate([key_weight, value_weight], axis=1)
    row_weight = jnp.concatenate([row_weight, lax.ppermute(row_weight, "tp", exchange)], axis=1)

    whole3 = lambda b, f: (0, 0, 0)
    by_block = pl.BlockSpec((block_rows, width), lambda b, f: (b, 0))
    d_queries, d_gates, pair_slots = pl.pallas_call(
        functools.partial(attend_kernel, per_block, span, heads),
        grid_spec=pltpu.PrefetchScalarGridSpec(
            num_scalar_prefetch=1,
            grid=(block_count,),
            in_specs=[by_block] * 4 + [pl.BlockSpec((slot_total, span, width), whole3)] * 2,
            out_specs=[
                by_block,
                by_block,
                pl.BlockSpec((slot_total, block_rows, heads * 2 * span), whole3),
            ],
        ),
        out_shape=[
            jax.ShapeDtypeStruct((tokens, width), bf16),
            jax.ShapeDtypeStruct((tokens, width), bf16),
            jax.ShapeDtypeStruct((slot_total, block_rows, heads * 2 * span), bf16),
        ],
        cost_estimate=pl.CostEstimate(flops=2_000_000_000, bytes_accessed=8_000_000, transcendentals=0),
        name="attend",
    )(slot_flat, queries, gates, output_grad, d_attended, came_keys, came_values)

    came_pairs = lax.all_to_all(
        pair_slots.reshape(owner_count, capacity, block_rows, heads * 2 * span),
        "st", split_axis=0, concat_axis=0, tiled=True,
    ).reshape(slot_total, block_rows, heads * 2 * span)

    unroll = 4 if slot_total % 4 == 0 else 1

    def shared_spec(u):
        return pl.BlockSpec(
            (1, block_rows, 2 * width), lambda i, p, r: (r[i * unroll + u], 0, 0)
        )

    key_low, value_low = pl.pallas_call(
        functools.partial(totals_kernel, unroll, heads, held, span),
        grid_spec=pltpu.PrefetchScalarGridSpec(
            num_scalar_prefetch=2,
            grid=(slot_total // unroll,),
            in_specs=[
                pl.BlockSpec((unroll, block_rows, heads * 2 * span), lambda i, p, r: (i, 0, 0))
            ]
            + [shared_spec(u) for u in range(unroll)],
            out_specs=[pl.BlockSpec((held, span, width), lambda i, p, r: (0, 0, 0))] * 2,
            scratch_shapes=[pltpu.VMEM((held + 1, span, width), f32)] * 2,
        ),
        out_shape=[jax.ShapeDtypeStruct((held, span, width), bf16)] * 2,
        cost_estimate=pl.CostEstimate(flops=2_000_000_000, bytes_accessed=8_000_000, transcendentals=0),
        name="totals",
    )(slot_target, slot_row, came_pairs, *([shared] * unroll))

    def over_heads(first, second, weight):
        rows = jnp.concatenate([first, second], axis=1)
        half = rows.shape[0] // tp_count
        theirs = lax.dynamic_slice_in_dim(rows, (tp_count - 1 - tp_index) * half, half, 0)
        mine = lax.dynamic_slice_in_dim(rows, tp_index * half, half, 0)
        got = lax.ppermute(theirs, "tp", exchange)
        both = jnp.concatenate([mine, got], axis=1)
        return lax.dot_general(both, weight, NT, preferred_element_type=f32).astype(bf16)

    grad_hidden = over_heads(d_queries, d_gates, token_weight)

    value_rows = value_low.reshape(held * span, width)
    weight_part = lax.dot_general(store_rows, value_rows, TN, preferred_element_type=f32)
    parts = lax.all_to_all(
        weight_part.astype(bf16).reshape(owner_count, model_width // owner_count, width),
        "st", split_axis=0, concat_axis=0, tiled=True,
    )
    weight_sum = jnp.sum(parts.astype(f32), axis=0)
    grad_value_weight = lax.all_gather(weight_sum, "st", axis=0, tiled=True)

    grad_store = over_heads(key_low.reshape(held * span, width), value_rows, row_weight).reshape(
        held // tp_count, span, model_width
    )
    return (grad_hidden, grad_store, grad_value_weight)


def solution(mesh):
    placed = (
        P("st", None),
        P("st", None, None),
        P("st", None),
        P(None, "tp"),
        P(None, "tp"),
        P(None, "tp"),
        P(None, "tp"),
        P("st", "tp"),
    )
    return jax.shard_map(
        body,
        mesh=mesh,
        in_specs=placed,
        out_specs=(P(("st", "tp"), None), P(("st", "tp"), None, None), P(None, "tp")),
        check_vma=False,
    )
```

```python
import functools

import jax
import jax.numpy as jnp
from jax import lax
from jax.experimental import pallas as pl
from jax.experimental.pallas import tpu as pltpu
from jax.sharding import PartitionSpec as P

HEAD_DIM = 256
NT = (((1,), (1,)), ((), ()))
TN = (((0,), (0,)), ((), ()))


def attend_kernel(per_block, span, heads, flat_ref, q_ref, gate_ref, up_ref, da_ref, k_ref, v_ref, dq_ref, dg_ref, dk_ref, dv_ref):
    b = pl.program_id(0)

    @pl.when(b == 0)
    def _():
        dk_ref[...] = jnp.zeros_like(dk_ref)
        dv_ref[...] = jnp.zeros_like(dv_ref)

    score_scale = HEAD_DIM ** (-0.5)
    slots = [flat_ref[b * per_block + j] for j in range(per_block)]
    keys = jnp.concatenate([k_ref[s] for s in slots], axis=0)
    values = jnp.concatenate([v_ref[s] for s in slots], axis=0)
    for h in range(heads):
        cols = slice(h * HEAD_DIM, (h + 1) * HEAD_DIM)
        k, v = keys[:, cols], values[:, cols]
        q, da = q_ref[:, cols], da_ref[:, cols]
        scores = lax.dot_general(q, k, NT, preferred_element_type=jnp.float32) * score_scale
        top = jnp.max(scores, axis=-1, keepdims=True)
        e = jnp.exp(scores - top)
        probs = e / jnp.sum(e, axis=-1, keepdims=True)
        probs_low = probs.astype(jnp.bfloat16)
        attended = jnp.dot(probs_low, v, preferred_element_type=jnp.float32)
        gates = gate_ref[:, cols]
        s = jax.nn.sigmoid(gates)
        up = up_ref[:, cols].astype(jnp.float32)
        dg_ref[:, cols] = (up * attended * s * (1.0 + gates * (1.0 - s))).astype(jnp.bfloat16)
        d_probs = lax.dot_general(da, v, NT, preferred_element_type=jnp.float32)
        centre = jnp.sum(probs * d_probs, axis=-1, keepdims=True)
        d_scores = (probs * (d_probs - centre) * score_scale).astype(jnp.bfloat16)
        dq_ref[:, cols] = jnp.dot(d_scores, k, preferred_element_type=jnp.float32).astype(
            jnp.bfloat16
        )
        d_keys = lax.dot_general(d_scores, q, TN, preferred_element_type=jnp.float32)
        d_values = lax.dot_general(probs_low, da, TN, preferred_element_type=jnp.float32)
        for j, slot in enumerate(slots):
            rows = slice(j * span, (j + 1) * span)
            dk_ref[slot, :, cols] = d_keys[rows].astype(jnp.bfloat16)
            dv_ref[slot, :, cols] = d_values[rows].astype(jnp.bfloat16)


def totals_kernel(unroll, held, passage_ref, came_ref, out_ref, acc):
    step = pl.program_id(0)

    @pl.when(step == 0)
    def _():
        acc[...] = jnp.zeros_like(acc)

    for u in range(unroll):
        acc[passage_ref[step * unroll + u]] += came_ref[u].astype(jnp.float32)

    @pl.when(step == pl.num_programs(0) - 1)
    def _():
        out_ref[...] = acc[:held].astype(jnp.bfloat16)


def body(
    hidden,
    passage_store,
    passage_ids,
    query_weight,
    gate_weight,
    key_weight,
    value_weight,
    output_grad,
):
    owner_count = lax.axis_size("st")
    tp_count = lax.axis_size("tp")
    tp_index = lax.axis_index("tp")
    held, span, model_width = passage_store.shape
    block_count, per_block = passage_ids.shape
    requests = block_count * per_block
    capacity = max(1, 2 * requests // owner_count)
    slot_total = owner_count * capacity
    width = query_weight.shape[1]
    heads = width // HEAD_DIM
    tokens = hidden.shape[0]
    block_rows = tokens // block_count
    bf16, f32 = jnp.bfloat16, jnp.float32
    exchange = [(i, tp_count - 1 - i) for i in range(tp_count)]

    ids = passage_ids.reshape(requests)
    owner_of = ids // held
    local_index = ids % held
    positions = jnp.arange(requests, dtype=jnp.int32)
    earlier = positions[None, :] < positions[:, None]
    rank = jnp.sum((owner_of[:, None] == owner_of[None, :]) & earlier, axis=1, dtype=jnp.int32)
    slot_flat = owner_of * capacity + rank
    code = local_index + 1
    hit = slot_flat[:, None] == jnp.arange(slot_total, dtype=jnp.int32)[None, :]
    table = jnp.sum(jnp.where(hit, code[:, None], 0), axis=0, dtype=jnp.int32)
    came = lax.all_to_all(
        table.reshape(owner_count, capacity), "st", split_axis=0, concat_axis=0, tiled=True
    ).reshape(slot_total)
    filled = came > 0
    slot_passage = jnp.maximum(came - 1, 0)
    slot_target = jnp.where(filled, slot_passage, held).astype(jnp.int32)

    store_rows = passage_store.reshape(held * span, model_width)

    def project(rows, weight):
        return jnp.dot(rows, weight, preferred_element_type=f32)

    keys_here = project(store_rows, key_weight).astype(bf16).reshape(held, span, width)
    values_here = project(store_rows, value_weight).astype(bf16).reshape(held, span, width)
    came_keys = lax.all_to_all(
        keys_here[slot_passage].reshape(owner_count, capacity, span, width),
        "st", split_axis=0, concat_axis=0, tiled=True,
    ).reshape(slot_total, span, width)
    came_values = lax.all_to_all(
        values_here[slot_passage].reshape(owner_count, capacity, span, width),
        "st", split_axis=0, concat_axis=0, tiled=True,
    ).reshape(slot_total, span, width)

    queries = project(hidden, query_weight).astype(bf16)
    gates = project(hidden, gate_weight)
    d_attended = (output_grad.astype(f32) * gates * jax.nn.sigmoid(gates)).astype(bf16)
    token_weight = jnp.concatenate([query_weight, gate_weight], axis=1)
    token_weight = jnp.concatenate(
        [token_weight, lax.ppermute(token_weight, "tp", exchange)], axis=1
    )
    row_weight = jnp.concatenate([key_weight, value_weight], axis=1)
    row_weight = jnp.concatenate([row_weight, lax.ppermute(row_weight, "tp", exchange)], axis=1)

    came_values, token_weight, row_weight = lax.optimization_barrier(
        (came_values, token_weight, row_weight)
    )

    whole3 = lambda b, f: (0, 0, 0)
    by_block = pl.BlockSpec((block_rows, width), lambda b, f: (b, 0))
    d_queries, d_gates, key_slots, value_slots = pl.pallas_call(
        functools.partial(attend_kernel, per_block, span, heads),
        grid_spec=pltpu.PrefetchScalarGridSpec(
            num_scalar_prefetch=1,
            grid=(block_count,),
            in_specs=[by_block] * 4 + [pl.BlockSpec((slot_total, span, width), whole3)] * 2,
            out_specs=[
                by_block,
                by_block,
                pl.BlockSpec((slot_total, span, width), whole3),
                pl.BlockSpec((slot_total, span, width), whole3),
            ],
        ),
        out_shape=[
            jax.ShapeDtypeStruct((tokens, width), bf16),
            jax.ShapeDtypeStruct((tokens, width), bf16),
            jax.ShapeDtypeStruct((slot_total, span, width), bf16),
            jax.ShapeDtypeStruct((slot_total, span, width), bf16),
        ],
        cost_estimate=pl.CostEstimate(flops=2_000_000_000, bytes_accessed=8_000_000, transcendentals=0),
        name="attend",
    )(slot_flat, queries, gates, output_grad, d_attended, came_keys, came_values)

    unroll = 8 if slot_total % 8 == 0 else 1

    def totals(slots):
        came = lax.all_to_all(
            slots.reshape(owner_count, capacity, span, width),
            "st", split_axis=0, concat_axis=0, tiled=True,
        ).reshape(slot_total, span, width)
        return pl.pallas_call(
            functools.partial(totals_kernel, unroll, held),
            grid_spec=pltpu.PrefetchScalarGridSpec(
                num_scalar_prefetch=1,
                grid=(slot_total // unroll,),
                in_specs=[pl.BlockSpec((unroll, span, width), lambda i, p: (i, 0, 0))],
                out_specs=pl.BlockSpec((held, span, width), lambda i, p: (0, 0, 0)),
                scratch_shapes=[pltpu.VMEM((held + 1, span, width), f32)],
            ),
            out_shape=jax.ShapeDtypeStruct((held, span, width), bf16),
            cost_estimate=pl.CostEstimate(
                flops=1_000_000_000, bytes_accessed=4_000_000, transcendentals=0
            ),
            name="totals",
        )(slot_target, came)

    value_low = totals(value_slots)
    key_low = totals(key_slots)

    def over_heads(first, second, weight):
        rows = jnp.concatenate([first, second], axis=1)
        half = rows.shape[0] // tp_count
        theirs = lax.dynamic_slice_in_dim(rows, (tp_count - 1 - tp_index) * half, half, 0)
        mine = lax.dynamic_slice_in_dim(rows, tp_index * half, half, 0)
        got = lax.ppermute(theirs, "tp", exchange)
        both = jnp.concatenate([mine, got], axis=1)
        return lax.dot_general(both, weight, NT, preferred_element_type=f32).astype(bf16)

    grad_hidden = over_heads(d_queries, d_gates, token_weight)

    value_rows = value_low.reshape(held * span, width)
    weight_part = lax.dot_general(store_rows, value_rows, TN, preferred_element_type=f32)
    parts = lax.all_to_all(
        weight_part.astype(bf16).reshape(owner_count, model_width // owner_count, width),
        "st", split_axis=0, concat_axis=0, tiled=True,
    )
    weight_sum = jnp.sum(parts.astype(f32), axis=0)
    shared = jnp.broadcast_to(weight_sum.astype(bf16)[None], parts.shape)
    grad_value_weight = (
        lax.all_to_all(shared, "st", split_axis=0, concat_axis=0, tiled=True)
        .reshape(model_width, width)
        .astype(f32)
    )

    grad_store = over_heads(key_low.reshape(held * span, width), value_rows, row_weight).reshape(
        held // tp_count, span, model_width
    )
    return (grad_hidden, grad_store, grad_value_weight)


def solution(mesh):
    placed = (
        P("st", None),
        P("st", None, None),
        P("st", None),
        P(None, "tp"),
        P(None, "tp"),
        P(None, "tp"),
        P(None, "tp"),
        P("st", "tp"),
    )
    return jax.shard_map(
        body,
        mesh=mesh,
        in_specs=placed,
        out_specs=(P(("st", "tp"), None), P(("st", "tp"), None, None), P(None, "tp")),
        check_vma=False,
    )
```
